32 devices in a mesh: sp: 16 (over z, y, x), tp: 2 (over core).
Axes of the slice: x: 2, y: 2, z: 4, core: 2. Of those that a mesh axis runs over, the one named last changes fastest.
Arguments:
- residual: bfloat16 [2048, 2048], P(('sp', 'tp')), may hold values from -6 to 6
- query_wide: bfloat16 [2048, 1024], P('sp', 'tp'), may hold values from -6 to 6
- key_wide: bfloat16 [2048, 1024], P('sp', 'tp'), may hold values from -6 to 6
- value_wide: bfloat16 [2048, 2048], P('sp', 'tp'), may hold values from -6 to 6
- outgate_wide: bfloat16 [2048, 2048], P('sp', 'tp'), may hold values from -6 to 6
- gating_wide: float32 [3, 8, 2048], P(None, 'tp', 'sp'), may hold values from -4 to 240, as said below
- gain_wide: bfloat16 [2048], P('tp'), may hold values from 0.099609375 to 1.8984375
- readout_wide: bfloat16 [2048, 2048], P('tp'), may hold values from -0.109375 to 0.109375
- query_narrow: bfloat16 [2048, 512], P('sp', 'tp'), may hold values from -6 to 6
- key_narrow: bfloat16 [2048, 512], P('sp', 'tp'), may hold values from -6 to 6
- value_narrow: bfloat16 [2048, 1024], P('sp', 'tp'), may hold values from -6 to 6
- outgate_narrow: bfloat16 [2048, 1024], P('sp', 'tp'), may hold values from -6 to 6
- gating_narrow: float32 [3, 8, 2048], P(None, 'tp', 'sp'), may hold values from -4 to 240, as said below
- gain_narrow: bfloat16 [1024], P('tp'), may hold values from 0.099609375 to 1.8984375
- readout_narrow: bfloat16 [1024, 2048], P('tp'), may hold values from -0.109375 to 0.109375
- norm_gain: bfloat16 [2048], replicated, may hold values from 0.099609375 to 1.8984375
- gate_weight: bfloat16 [2048, 5632], P('sp', 'tp'), may hold values from -0.125 to 0.125
- up_weight: bfloat16 [2048, 5632], P('sp', 'tp'), may hold values from -0.125 to 0.125
- down_weight: bfloat16 [5632, 2048], P('tp', 'sp'), may hold values from -0.078125 to 0.078125
Outputs:
- mixed_out: bfloat16 [2048, 2048], P(('sp', 'tp'))
The draws below stay inside these ranges and needn't reach their ends.
Inputs may be any that keep to these rules, and one draw needn't show every extreme that they name: `gating_wide`: row 0 holds input gate pre-activations, row 1 forget gate pre-activations, row 2 an added log-decay that is zero or negative. `gating_narrow`: row 0 holds input gate pre-activations, row 1 forget gate pre-activations, row 2 an added log-decay that is zero or negative.
All inputs are finite; a program needn't handle non-finite values.
Results may differ from the reference program's by a relative error of at most 0.017.
Values may be sent and summed in bfloat16 or wider, within the bound.
A program may use at most 128 MiB of HBM per device.

```python
import math
import jax
import jax.numpy as jnp
from jax import lax

D = 2048
FF = 5632
HEADS_A = 8
DK_A = 128
DV_A = 256
HEADS_B = 8
DK_B = 64
DV_B = 128
BLOCK = 64
TOK_DEV = 128
CONTEXT_LENGTH = 2048
N_TP = 2


def draw_gating(key, attention_tally):
    keys = jax.random.split(key, 10)
    incoming_matrix = jnp.clip(jax.random.normal(keys[0], (attention_tally, CONTEXT_LENGTH), jnp.float32), -4.0, 4.0)
    entry_ordinal = jnp.broadcast_to(jnp.arange(attention_tally)[:, None], (attention_tally, 4))
    threshold = 50
    fast = jax.random.randint(keys[5], (attention_tally,), 0, 100) < threshold
    base = jnp.where(fast, 4.0, math.log(CONTEXT_LENGTH) + 1.0)
    levels = jnp.repeat(jax.random.uniform(keys[6], (CONTEXT_LENGTH // TOK_DEV,), jnp.float32, -0.7, 0.7), TOK_DEV)
    jitter = jax.random.uniform(keys[7], (attention_tally, CONTEXT_LENGTH), jnp.float32, -1.0, 1.0)
    retention_factor = base[:, None] + levels[None, :] + jitter
    word_locations = jax.random.randint(keys[8], (attention_tally, 3), 0, CONTEXT_LENGTH)
    objective_scores = jnp.log(jax.random.uniform(keys[9], (attention_tally, 3), jnp.float32, 0.5, 0.8))
    admission_exponent = jnp.zeros((attention_tally, CONTEXT_LENGTH), jnp.float32).at[entry_ordinal[:, :3], word_locations].add(objective_scores)
    admission_exponent = jnp.maximum(admission_exponent, -4.0)
    return jnp.stack([incoming_matrix, retention_factor, admission_exponent])


def draw_gating_wide(key, part):
    return draw_gating(jax.random.fold_in(key, 11), HEADS_A)


def draw_gating_narrow(key, part):
    return draw_gating(jax.random.fold_in(key, 12), HEADS_B)


def steps_of(own_key, extent, cuts, low, largest):
    level, own = 1.0, jax.random.fold_in(own_key, 6)
    for position, shards_of in cuts:
        draws = jnp.exp(jax.random.uniform(jax.random.fold_in(own, position), (shards_of,), jnp.float32, low / len(cuts), largest / len(cuts)))
        level = level * jnp.repeat(draws, extent[position] // shards_of).reshape([-1 if axis == position else 1 for axis in range(len(extent))])
    return level


def scatter_about(key, shape, width, bound, pieces=(), kind=jnp.bfloat16):
    array = jax.random.normal(key, shape, jnp.float32) * width
    if len(pieces) > 0:
        array = steps_of(key, shape, pieces, -0.22, 0.18) * array
    return jnp.clip(array, min=-bound, max=bound).astype(kind)


def setup_inputs(seed: int = 0) -> dict:
    splits = jax.random.split(jax.random.key(seed), 20)
    return {
        "residual": scatter_about(splits[0], (CONTEXT_LENGTH, D), 1.0, 6.0, ((0, 32),)),
        "query_wide": scatter_about(splits[1], (CONTEXT_LENGTH, HEADS_A * DK_A), 1.0, 6.0, ((0, 16), (1, 2))),
        "key_wide": scatter_about(splits[2], (CONTEXT_LENGTH, HEADS_A * DK_A), 1.0, 6.0, ((0, 16), (1, 2))),
        "value_wide": scatter_about(splits[3], (CONTEXT_LENGTH, HEADS_A * DV_A), 1.0, 6.0, ((0, 16), (1, 2))),
        "outgate_wide": scatter_about(splits[4], (CONTEXT_LENGTH, HEADS_A * DV_A), 1.0, 6.0, ((0, 16), (1, 2))),
        "gating_wide": draw_gating_wide(jax.random.fold_in(splits[19], 71), 0),
        "gain_wide": jnp.clip(1.0 + 0.18 * jax.random.normal(splits[6], (HEADS_A * DV_A,), jnp.float32), 0.099609375, 1.8984375).astype(jnp.bfloat16),
        "readout_wide": scatter_about(splits[7], (HEADS_A * DV_A, D), (HEADS_A * DV_A + HEADS_B * DV_B) ** -0.5, 0.109375, ((0, 2),)),
        "query_narrow": scatter_about(splits[8], (CONTEXT_LENGTH, HEADS_B * DK_B), 1.0, 6.0, ((0, 16), (1, 2))),
        "key_narrow": scatter_about(splits[9], (CONTEXT_LENGTH, HEADS_B * DK_B), 1.0, 6.0, ((0, 16), (1, 2))),
        "value_narrow": scatter_about(splits[10], (CONTEXT_LENGTH, HEADS_B * DV_B), 1.0, 6.0, ((0, 16), (1, 2))),
        "outgate_narrow": scatter_about(splits[11], (CONTEXT_LENGTH, HEADS_B * DV_B), 1.0, 6.0, ((0, 16), (1, 2))),
        "gating_narrow": draw_gating_narrow(jax.random.fold_in(splits[19], 71), 0),
        "gain_narrow": jnp.clip(1.0 + 0.18 * jax.random.normal(splits[13], (HEADS_B * DV_B,), jnp.float32), 0.099609375, 1.8984375).astype(jnp.bfloat16),
        "readout_narrow": scatter_about(splits[14], (HEADS_B * DV_B, D), (HEADS_A * DV_A + HEADS_B * DV_B) ** -0.5, 0.109375, ((0, 2),)),
        "norm_gain": jnp.clip(1.0 + 0.18 * jax.random.normal(splits[15], (D,), jnp.float32), 0.099609375, 1.8984375).astype(jnp.bfloat16),
        "gate_weight": scatter_about(splits[16], (D, FF), D ** -0.5, 0.125, ((0, 16), (1, 2))),
        "up_weight": scatter_about(splits[17], (D, FF), D ** -0.5, 0.125, ((0, 16), (1, 2))),
        "down_weight": scatter_about(splits[18], (FF, D), FF ** -0.5, 0.078125, ((0, 2), (1, 16))),
    }


def block_scan(query, key_rows, value, gating):
    tokens = query.shape[0]
    attention_tally = gating.shape[1]
    key_size = query.shape[1] // attention_tally
    value_size = value.shape[1] // attention_tally
    nblocks = tokens // BLOCK
    scale = key_size ** (-0.5)
    queries = query.astype(jnp.float32).reshape(nblocks, BLOCK, attention_tally, key_size)
    keys_all = key_rows.astype(jnp.float32).reshape(nblocks, BLOCK, attention_tally, key_size)
    values_all = value.astype(jnp.float32).reshape(nblocks, BLOCK, attention_tally, value_size)
    incoming_matrix = jnp.moveaxis(gating[0].reshape(attention_tally, nblocks, BLOCK), 1, 0)
    forget_log = jax.nn.log_sigmoid(gating[1]) + gating[2]
    forgets = jnp.moveaxis(forget_log.reshape(attention_tally, nblocks, BLOCK), 1, 0)
    causal = jnp.tril(jnp.ones((BLOCK, BLOCK), dtype=bool))

    def advance(carry, blocks):
        memory, level = carry
        q_block, k_block, v_block, in_block, f_block = blocks
        cumul = jnp.cumsum(f_block, axis=-1)
        logits = cumul[:, :, None] - cumul[:, None, :] + in_block[:, None, :]
        logits = jnp.where(causal, logits, -jnp.inf)
        carried = cumul + level[:, None]
        stab = jnp.maximum(carried, lax.optimization_barrier(jnp.max(logits, axis=-1)))
        weights = jnp.exp(logits - stab[:, :, None])
        scores = jnp.einsum('thd,shd->hts', q_block, k_block) * scale
        weighted = (scores * weights).astype(jnp.bfloat16).astype(jnp.float32)
        within = jnp.einsum('hts,shv->thv', weighted, v_block)
        earlier = jnp.einsum('thd,hdv->thv', q_block, memory, precision=lax.Precision.HIGHEST)
        earlier = earlier * jnp.exp(carried - stab).T[:, :, None]
        last = cumul[:, -1]
        tail = last[:, None] - cumul + in_block
        level_new = jnp.maximum(last + level, lax.optimization_barrier(jnp.max(tail, axis=-1)))
        tail_weights = jnp.exp(tail - level_new[:, None]) * scale
        scaled_keys = (k_block * tail_weights.T[:, :, None]).astype(jnp.bfloat16).astype(jnp.float32)
        memory_new = jnp.exp(last + level - level_new)[:, None, None] * memory
        memory_new = memory_new + jnp.einsum('shd,shv->hdv', scaled_keys, v_block)
        return ((memory_new, level_new), within + earlier)
    init = (jnp.zeros((attention_tally, key_size, value_size), jnp.float32), jnp.full((attention_tally,), -1e+30, jnp.float32))
    _, raw = lax.scan(advance, init, (queries, keys_all, values_all, incoming_matrix, forgets))
    return raw.reshape(tokens, attention_tally, value_size)

def finish(raw, gain, outgate):
    tokens, attention_tally, value_size = raw.shape
    normal_raw = raw * lax.rsqrt(lax.optimization_barrier(jnp.mean(raw * raw, axis=-1, keepdims=True)) + 1e-06)
    flat = normal_raw.reshape(tokens, attention_tally * value_size)
    flat = flat * gain.astype(jnp.float32) * jax.nn.sigmoid(outgate.astype(jnp.float32))
    return flat.astype(jnp.bfloat16)

def reference(residual, query_wide, key_wide, value_wide, outgate_wide, gating_wide, gain_wide, readout_wide, query_narrow, key_narrow, value_narrow, outgate_narrow, gating_narrow, gain_narrow, readout_narrow, norm_gain, gate_weight, up_weight, down_weight):
    gated_wide = finish(block_scan(query_wide, key_wide, value_wide, gating_wide), gain_wide, outgate_wide)
    gated_narrow = finish(block_scan(query_narrow, key_narrow, value_narrow, gating_narrow), gain_narrow, outgate_narrow)
    span_wide = gated_wide.shape[1] // N_TP
    span_narrow = gated_narrow.shape[1] // N_TP
    mixed = jnp.zeros(residual.shape, jnp.float32)
    for index in range(N_TP):
        part = jnp.dot(gated_wide[:, index * span_wide:(index + 1) * span_wide], readout_wide[index * span_wide:(index + 1) * span_wide], preferred_element_type=jnp.float32)
        part = part + jnp.dot(gated_narrow[:, index * span_narrow:(index + 1) * span_narrow], readout_narrow[index * span_narrow:(index + 1) * span_narrow], preferred_element_type=jnp.float32)
        mixed = mixed + part.astype(jnp.bfloat16).astype(jnp.float32)
    middle = (residual.astype(jnp.float32) + mixed).astype(jnp.bfloat16)
    middle_f = middle.astype(jnp.float32)
    normed = middle_f * lax.rsqrt(lax.optimization_barrier(jnp.mean(middle_f * middle_f, axis=-1, keepdims=True)) + 1e-06)
    normed = (normed * norm_gain.astype(jnp.float32)).astype(jnp.bfloat16)
    hidden_span = FF // N_TP
    back = jnp.zeros(residual.shape, jnp.float32)
    for index in range(N_TP):
        cols = slice(index * hidden_span, (index + 1) * hidden_span)
        gate = jnp.dot(normed, gate_weight[:, cols], preferred_element_type=jnp.float32)
        upper = jnp.dot(normed, up_weight[:, cols], preferred_element_type=jnp.float32)
        hidden = (jax.nn.silu(gate) * upper).astype(jnp.bfloat16)
        part = jnp.dot(hidden, down_weight[cols], preferred_element_type=jnp.float32)
        back = back + part.astype(jnp.bfloat16).astype(jnp.float32)
    return (middle_f + back).astype(jnp.bfloat16)
```

```python
import functools

import jax
import jax.numpy as jnp
from jax import lax
from jax.experimental import pallas as pl
from jax.experimental.pallas import tpu as pltpu
from jax.sharding import Mesh, PartitionSpec as P

DK_A = 128
DK_B = 64
LOW = -1e30
MESH = pl.DeviceIdType.MESH


def cell_kernel(
    n,
    q_w,
    k_w,
    v_w,
    og_w,
    gain_w,
    q_n,
    k_n,
    v_n,
    og_n,
    gain_n,
    gating,
    out_w,
    out_n,
    raw_w,
    raw_n,
    stabs,
    sent,
    got,
    back,
    carried,
    mem_w,
    mem_n,
    state,
    levels,
    send_sem,
    recv_sem,
    send_sem2,
    recv_sem2,
):
    na, nb = lax.axis_size("a"), lax.axis_size("b")
    tp = lax.axis_index("tp")
    me = lax.axis_index("a") * nb + lax.axis_index("b")

    def where_is(index):
        return (index // nb, lax.rem(index, nb), tp)

    barrier = pltpu.get_barrier_semaphore()

    def greet(r, _):
        peer = lax.rem(me + r, n)
        pl.semaphore_signal(barrier, inc=1, device_id=where_is(peer), device_id_type=MESH)
        return 0

    lax.fori_loop(1, n, greet, 0)

    rows = q_w.shape[0]
    heads_p = gating.shape[1]
    groups = (
        (q_w, k_w, v_w, og_w, gain_w, out_w, raw_w, mem_w, DK_A),
        (q_n, k_n, v_n, og_n, gain_n, out_n, raw_n, mem_n, DK_B),
    )
    heads = tuple(g[0].shape[1] // g[8] for g in groups)
    parts = tuple(h * g[8] // n for h, g in zip(heads, groups))
    starts = (0, parts[0])
    extra = parts[0] + parts[1]

    it = lax.broadcasted_iota(jnp.int32, (rows, rows), 0)
    js = lax.broadcasted_iota(jnp.int32, (rows, rows), 1)
    upper = (it <= js).astype(jnp.float32)
    eye = (it == js).astype(jnp.float32)
    last_dims = (((1,), (1,)), ((), ()))
    first_dims = (((0,), (0,)), ((), ()))
    gate_in = gating[0]
    x = gating[1]
    forget = jnp.minimum(x, 0.0) - jnp.log1p(jnp.exp(-jnp.abs(x))) + gating[2]
    cum = jnp.dot(
        forget, upper, precision=lax.Precision.HIGHEST, preferred_element_type=jnp.float32
    )
    cum_t = lax.dot_general(
        eye, cum, last_dims, precision=lax.Precision.HIGHEST, preferred_element_type=jnp.float32
    )
    diff = gate_in - cum
    diff_t = lax.dot_general(
        eye, diff, last_dims, precision=lax.Precision.HIGHEST, preferred_element_type=jnp.float32
    )
    total = cum[:, rows - 1 : rows]
    level = jnp.max(total + diff, axis=1, keepdims=True)
    total_t = cum_t[rows - 1 : rows, :]
    level_t = jnp.max(total_t + diff_t, axis=0, keepdims=True)
    tail_t = jnp.exp(total_t + diff_t - level_t)
    width = sent.shape[2]
    lane = lax.broadcasted_iota(jnp.int32, (heads_p, width), 1)
    marks = jnp.where(
        lane < width // 2,
        jnp.broadcast_to(level, (heads_p, width)),
        jnp.broadcast_to(total, (heads_p, width)),
    )

    index = 0
    for g, (q, k, v, _, _, _, raw, _, dk) in enumerate(groups):
        dv = v.shape[1] // heads[g]
        scale = dk ** (-0.5)
        for h in range(heads[g]):
            k_h = k[:, h * dk : (h + 1) * dk]
            v_h = v[:, h * dv : (h + 1) * dv]
            scaled = k_h.astype(jnp.float32) * (tail_t[:, index : index + 1] * scale)
            memory = lax.dot_general(
                scaled.astype(jnp.bfloat16), v_h, first_dims, preferred_element_type=jnp.float32
            )
            size = parts[g]
            per = dk // size
            for p in range(per):
                sent[h * per + p, starts[g] : starts[g] + size, :dv] = memory[
                    p * size : (p + 1) * size
                ]
            index += 1
    spare = v_n.shape[1] // heads[1]
    if spare < width:
        sent[:, starts[1] : extra, spare:] = jnp.zeros((n, parts[1], width - spare), jnp.float32)
    for p in range(n):
        sent[p, extra : extra + heads_p, :] = marks

    pl.semaphore_wait(barrier, n - 1)

    def out_copy(r):
        peer = lax.rem(me + r, n)
        return pltpu.make_async_remote_copy(
            src_ref=sent.at[peer],
            dst_ref=got.at[me],
            send_sem=send_sem.at[r],
            recv_sem=recv_sem.at[r],
            device_id=where_is(peer),
            device_id_type=MESH,
        )

    lax.fori_loop(1, n, lambda r, c: (out_copy(r).start(), c)[1], 0)
    got[me] = sent[me]

    index = 0
    for g, (q, k, v, _, _, _, raw, _, dk) in enumerate(groups):
        dv = v.shape[1] // heads[g]
        scale = dk ** (-0.5)
        for h in range(heads[g]):
            q_h = q[:, h * dk : (h + 1) * dk]
            k_h = k[:, h * dk : (h + 1) * dk]
            v_h = v[:, h * dv : (h + 1) * dv]
            scores = lax.dot_general(q_h, k_h, last_dims, preferred_element_type=jnp.float32)
            logits = cum_t[:, index : index + 1] + diff[index : index + 1, :]
            logits = jnp.where(js <= it, logits, LOW)
            stab = jnp.max(logits, axis=1, keepdims=True)
            weighted = scores * scale * jnp.exp(logits - stab)
            raw[:, h * dv : (h + 1) * dv] = jnp.dot(
                weighted.astype(jnp.bfloat16), v_h, preferred_element_type=jnp.float32
            )
            stabs[:, index : index + 1] = stab
            index += 1

    lax.fori_loop(1, n, lambda r, c: (out_copy(r).wait(), c)[1], 0)

    which = tuple(
        (me * parts[g]) // groups[g][8] + (heads[0] if g else 0) for g in range(2)
    )
    sub = lax.broadcasted_iota(jnp.int32, (heads_p, width), 0)
    picks = tuple(sub == w for w in which)

    def merge(t, _):
        level_c = levels[0]
        back[t] = state[...]
        levels[1] = jnp.where(t == me, level_c, levels[1])
        mark = got[t, extra : extra + heads_p, :]
        lev = jnp.broadcast_to(mark[:, :1], mark.shape)
        tot = jnp.broadcast_to(mark[:, width - 1 :], mark.shape)
        new = jnp.maximum(level_c + tot, lev)
        old_f = jnp.exp(level_c + tot - new)
        new_f = jnp.exp(lev - new)
        levels[0] = new
        for g in range(2):
            span = slice(starts[g], starts[g] + parts[g])

            def pick(f):
                return jnp.sum(jnp.where(picks[g], f, 0.0), axis=0, keepdims=True)

            state[span, :] = pick(old_f) * state[span, :] + pick(new_f) * got[t, span, :]
        return 0

    levels[...] = jnp.full(levels.shape, LOW, jnp.float32)
    state[...] = jnp.zeros(state.shape, jnp.float32)
    lax.fori_loop(0, n, merge, 0)
    entering = levels[1]

    def back_copy(r):
        peer = lax.rem(me + r, n)
        return pltpu.make_async_remote_copy(
            src_ref=back.at[peer],
            dst_ref=carried.at[me],
            send_sem=send_sem2.at[r],
            recv_sem=recv_sem2.at[r],
            device_id=where_is(peer),
            device_id_type=MESH,
        )

    lax.fori_loop(1, n, lambda r, c: (back_copy(r).start(), c)[1], 0)
    carried[me] = back[me]
    entering_t = lax.dot_general(
        jnp.where(
            lax.broadcasted_iota(jnp.int32, (rows, width), 1) == 0, 1.0, 0.0
        ),
        entering,
        last_dims,
        precision=lax.Precision.HIGHEST,
        preferred_element_type=jnp.float32,
    )
    shifted = cum_t + entering_t
    own = stabs[:, :heads_p]
    both = jnp.maximum(own, shifted)
    own_f = jnp.exp(own - both)
    in_f = jnp.exp(shifted - both)
    lax.fori_loop(1, n, lambda r, c: (back_copy(r).wait(), c)[1], 0)

    index = 0
    for g, (q, _, v, og, gain, out, raw, mem, dk) in enumerate(groups):
        dv = v.shape[1] // heads[g]
        size = parts[g]
        per = dk // size
        for h in range(heads[g]):
            for p in range(per):
                mem[p * size : (p + 1) * size, :] = carried[
                    h * per + p, starts[g] : starts[g] + size, :dv
                ]
            memory = mem[...]
            high = memory.astype(jnp.bfloat16)
            rest = (memory - high.astype(jnp.float32)).astype(jnp.bfloat16)
            q_h = q[:, h * dk : (h + 1) * dk]
            cols = slice(h * dv, (h + 1) * dv)
            incoming = jnp.dot(q_h, high, preferred_element_type=jnp.float32) + jnp.dot(
                q_h, rest, preferred_element_type=jnp.float32
            )
            value = (
                raw[:, cols] * own_f[:, index : index + 1]
                + incoming * in_f[:, index : index + 1]
            )
            value = value * lax.rsqrt(jnp.mean(value * value, axis=1, keepdims=True) + 1e-06)
            gate = 1.0 / (1.0 + jnp.exp(-og[:, cols].astype(jnp.float32)))
            value = value * gain[:, cols].astype(jnp.float32) * gate
            out[:, cols] = value.astype(jnp.bfloat16)
            index += 1


def cell(q_w, k_w, v_w, og_w, gat_w, gain_w, q_n, k_n, v_n, og_n, gat_n, gain_n):
    n = lax.axis_size("a") * lax.axis_size("b")
    rows = q_w.shape[0]
    heads = gat_w.shape[1] + gat_n.shape[1]
    heads_p = -(-heads // 8) * 8
    gating = jnp.concatenate([gat_w, gat_n], axis=1)
    gating = jnp.pad(gating, ((0, 0), (0, heads_p - heads), (0, 0)))
    parts = (q_w.shape[1] // n, q_n.shape[1] // n)
    width = v_w.shape[1] // gat_w.shape[1]
    width_n = v_n.shape[1] // gat_n.shape[1]
    vmem = pl.BlockSpec(memory_space=pltpu.VMEM)
    state = parts[0] + parts[1]
    return pl.pallas_call(
        functools.partial(cell_kernel, n),
        out_shape=(
            jax.ShapeDtypeStruct(v_w.shape, jnp.bfloat16),
            jax.ShapeDtypeStruct(v_n.shape, jnp.bfloat16),
        ),
        in_specs=[vmem] * 11,
        out_specs=(vmem, vmem),
        scratch_shapes=[
            pltpu.VMEM(v_w.shape, jnp.float32),
            pltpu.VMEM(v_n.shape, jnp.float32),
            pltpu.VMEM((rows, 128), jnp.float32),
            pltpu.VMEM((n, state + heads_p, width), jnp.float32),
            pltpu.VMEM((n, state + heads_p, width), jnp.float32),
            pltpu.VMEM((n, state, width), jnp.float32),
            pltpu.VMEM((n, state, width), jnp.float32),
            pltpu.VMEM((DK_A, width), jnp.float32),
            pltpu.VMEM((DK_B, width_n), jnp.float32),
            pltpu.VMEM((state, width), jnp.float32),
            pltpu.VMEM((2, heads_p, width), jnp.float32),
            pltpu.SemaphoreType.DMA((n,)),
            pltpu.SemaphoreType.DMA((n,)),
            pltpu.SemaphoreType.DMA((n,)),
            pltpu.SemaphoreType.DMA((n,)),
        ],
        compiler_params=pltpu.CompilerParams(
            collective_id=0, has_side_effects=True, vmem_limit_bytes=32 * 2**20
        ),
        cost_estimate=pl.CostEstimate(
            flops=2 * 10**9, bytes_accessed=120 * 10**6, transcendentals=0
        ),
    )(
        q_w,
        k_w,
        v_w,
        og_w,
        gain_w.reshape(1, -1),
        q_n,
        k_n,
        v_n,
        og_n,
        gain_n.reshape(1, -1),
        gating,
    )


def body(
    residual,
    query_wide,
    key_wide,
    value_wide,
    outgate_wide,
    gating_wide,
    gain_wide,
    readout_wide,
    query_narrow,
    key_narrow,
    value_narrow,
    outgate_narrow,
    gating_narrow,
    gain_narrow,
    readout_narrow,
    norm_gain,
    gate_weight,
    up_weight,
    down_weight,
):
    na, nb = lax.axis_size("a"), lax.axis_size("b")
    depth, hidden_tp = gate_weight.shape
    chunk = hidden_tp // na
    out_cols = down_weight.shape[1]
    model = residual.shape[1]

    def regroup(pieces):
        mine = lax.all_to_all(pieces, "a", split_axis=0, concat_axis=0, tiled=True)
        return lax.all_gather(mine, "b", axis=0, tiled=True)

    gate_all = regroup(jnp.moveaxis(gate_weight.reshape(depth, na, chunk), 1, 0))
    up_all = regroup(jnp.moveaxis(up_weight.reshape(depth, na, chunk), 1, 0))
    down_all = regroup(down_weight.reshape(na, chunk, out_cols))

    gated_w, gated_n = cell(
        query_wide,
        key_wide,
        value_wide,
        outgate_wide,
        gating_wide,
        gain_wide,
        query_narrow,
        key_narrow,
        value_narrow,
        outgate_narrow,
        gating_narrow,
        gain_narrow,
    )
    mixed = lax.psum_scatter(
        (
            jnp.dot(gated_w, readout_wide, preferred_element_type=jnp.float32)
            + jnp.dot(gated_n, readout_narrow, preferred_element_type=jnp.float32)
        ).astype(jnp.bfloat16),
        "tp",
        scatter_dimension=0,
        tiled=True,
    ).astype(jnp.float32)
    middle_f = (residual.astype(jnp.float32) + mixed).astype(jnp.bfloat16).astype(jnp.float32)
    normed = middle_f * lax.rsqrt(jnp.mean(middle_f * middle_f, axis=-1, keepdims=True) + 1e-06)
    normed = (normed * norm_gain.astype(jnp.float32)).astype(jnp.bfloat16)
    own_rows = normed.shape[0]
    normed = normed.reshape(own_rows, na, nb, depth).swapaxes(1, 2).reshape(own_rows, model)
    all_rows = lax.all_gather(normed, ("a", "tp"), axis=0, tiled=True)
    gate = jnp.dot(all_rows, gate_all.reshape(model, chunk), preferred_element_type=jnp.float32)
    upper = jnp.dot(all_rows, up_all.reshape(model, chunk), preferred_element_type=jnp.float32)
    hidden = (jax.nn.silu(gate) * upper).astype(jnp.bfloat16)
    down = jnp.transpose(down_all, (1, 0, 2)).reshape(chunk, model)
    terms = jnp.dot(hidden, down, preferred_element_type=jnp.float32)
    back = lax.psum_scatter(
        terms.astype(jnp.bfloat16), ("a", "tp"), scatter_dimension=0, tiled=True
    ).astype(jnp.float32)
    back = back.reshape(own_rows, nb, na, out_cols).swapaxes(1, 2).reshape(own_rows, model)
    return (middle_f + back).astype(jnp.bfloat16)


def solution(mesh):
    sp, tp = mesh.shape["sp"], mesh.shape["tp"]
    a = 4 if sp % 4 == 0 else 1
    split = Mesh(mesh.devices.reshape(a, sp // a, tp), ("a", "b", "tp"))
    s = ("a", "b")
    in_specs = (
        P(("a", "b", "tp"), None),
        P(s, "tp"),
        P(s, "tp"),
        P(s, "tp"),
        P(s, "tp"),
        P(None, "tp", s),
        P("tp"),
        P("tp", None),
        P(s, "tp"),
        P(s, "tp"),
        P(s, "tp"),
        P(s, "tp"),
        P(None, "tp", s),
        P("tp"),
        P("tp", None),
        P(),
        P(s, "tp"),
        P(s, "tp"),
        P("tp", s),
    )
    out_specs = P(("a", "b", "tp"), None)
    return jax.shard_map(body, mesh=split, in_specs=in_specs, out_specs=out_specs, check_vma=False)
```

```python
import functools

import jax
import jax.numpy as jnp
from jax import lax
from jax.experimental import pallas as pl
from jax.experimental.pallas import tpu as pltpu
from jax.sharding import Mesh, PartitionSpec as P

DK_A = 128
DK_B = 64
LOW = -1e30
MESH = pl.DeviceIdType.MESH


def cell_kernel(
    n,
    q_w,
    k_w,
    v_w,
    og_w,
    gain_w,
    q_n,
    k_n,
    v_n,
    og_n,
    gain_n,
    gating,
    gate_in_w,
    up_in_w,
    down_in_w,
    out_w,
    out_n,
    gate_all,
    up_all,
    down_all,
    raw_w,
    raw_n,
    stabs,
    sent,
    got,
    back,
    carried,
    mem_w,
    mem_n,
    state,
    levels,
    send_sem,
    recv_sem,
    send_sem2,
    recv_sem2,
    send_sem3,
    recv_sem3,
    own_sem,
):
    na, nb = lax.axis_size("a"), lax.axis_size("b")
    tp = lax.axis_index("tp")
    me = lax.axis_index("a") * nb + lax.axis_index("b")

    def where_is(index):
        return (index // nb, lax.rem(index, nb), tp)

    barrier = pltpu.get_barrier_semaphore()

    def greet(r, _):
        peer = lax.rem(me + r, n)
        pl.semaphore_signal(barrier, inc=1, device_id=where_is(peer), device_id_type=MESH)
        return 0

    lax.fori_loop(1, n, greet, 0)

    rows = q_w.shape[0]
    heads_p = gating.shape[1]
    groups = (
        (q_w, k_w, v_w, og_w, gain_w, out_w, raw_w, mem_w, DK_A),
        (q_n, k_n, v_n, og_n, gain_n, out_n, raw_n, mem_n, DK_B),
    )
    heads = tuple(g[0].shape[1] // g[8] for g in groups)
    parts = tuple(h * g[8] // n for h, g in zip(heads, groups))
    starts = (0, parts[0])
    extra = parts[0] + parts[1]

    it = lax.broadcasted_iota(jnp.int32, (rows, rows), 0)
    js = lax.broadcasted_iota(jnp.int32, (rows, rows), 1)
    upper = (it <= js).astype(jnp.float32)
    eye = (it == js).astype(jnp.float32)
    last_dims = (((1,), (1,)), ((), ()))
    first_dims = (((0,), (0,)), ((), ()))
    gate_in = gating[0]
    x = gating[1]
    forget = jnp.minimum(x, 0.0) - jnp.log1p(jnp.exp(-jnp.abs(x))) + gating[2]
    cum = jnp.dot(
        forget, upper, precision=lax.Precision.HIGHEST, preferred_element_type=jnp.float32
    )
    cum_t = lax.dot_general(
        eye, cum, last_dims, precision=lax.Precision.HIGHEST, preferred_element_type=jnp.float32
    )
    diff = gate_in - cum
    diff_t = lax.dot_general(
        eye, diff, last_dims, precision=lax.Precision.HIGHEST, preferred_element_type=jnp.float32
    )
    total = cum[:, rows - 1 : rows]
    level = jnp.max(total + diff, axis=1, keepdims=True)
    total_t = cum_t[rows - 1 : rows, :]
    level_t = jnp.max(total_t + diff_t, axis=0, keepdims=True)
    tail_t = jnp.exp(total_t + diff_t - level_t)
    width = sent.shape[2]
    lane = lax.broadcasted_iota(jnp.int32, (heads_p, width), 1)
    marks = jnp.where(
        lane < width // 2,
        jnp.broadcast_to(level, (heads_p, width)),
        jnp.broadcast_to(total, (heads_p, width)),
    )

    index = 0
    for g, (q, k, v, _, _, _, raw, _, dk) in enumerate(groups):
        dv = v.shape[1] // heads[g]
        scale = dk ** (-0.5)
        for h in range(heads[g]):
            k_h = k[:, h * dk : (h + 1) * dk]
            v_h = v[:, h * dv : (h + 1) * dv]
            scaled = k_h.astype(jnp.float32) * (tail_t[:, index : index + 1] * scale)
            memory = lax.dot_general(
                scaled.astype(jnp.bfloat16), v_h, first_dims, preferred_element_type=jnp.float32
            )
            size = parts[g]
            per = dk // size
            for p in range(per):
                sent[h * per + p, starts[g] : starts[g] + size, :dv] = memory[
                    p * size : (p + 1) * size
                ]
            index += 1
    spare = v_n.shape[1] // heads[1]
    if spare < width:
        sent[:, starts[1] : extra, spare:] = jnp.zeros((n, parts[1], width - spare), jnp.float32)
    for p in range(n):
        sent[p, extra : extra + heads_p, :] = marks

    pl.semaphore_wait(barrier, n - 1)

    def out_copy(r):
        peer = lax.rem(me + r, n)
        return pltpu.make_async_remote_copy(
            src_ref=sent.at[peer],
            dst_ref=got.at[me],
            send_sem=send_sem.at[r],
            recv_sem=recv_sem.at[r],
            device_id=where_is(peer),
            device_id_type=MESH,
        )

    lax.fori_loop(1, n, lambda r, c: (out_copy(r).start(), c)[1], 0)
    weights = ((gate_in_w, gate_all), (up_in_w, up_all), (down_in_w, down_all))

    def weight_copy(w, r):
        peer = lax.rem(me + r, n)
        return pltpu.make_async_remote_copy(
            src_ref=weights[w][0].at[peer // nb],
            dst_ref=weights[w][1].at[me],
            send_sem=send_sem3.at[w, r],
            recv_sem=recv_sem3.at[w, r],
            device_id=where_is(peer),
            device_id_type=MESH,
        )

    def own_copy(w):
        return pltpu.make_async_copy(
            weights[w][0].at[lax.axis_index("a")], weights[w][1].at[me], own_sem.at[w]
        )

    def start_two(r, _):
        weight_copy(0, r).start()
        weight_copy(1, r).start()
        return 0

    lax.fori_loop(1, n, start_two, 0)
    for w in range(3):
        own_copy(w).start()
    got[me] = sent[me]

    index = 0
    for g, (q, k, v, _, _, _, raw, _, dk) in enumerate(groups):
        dv = v.shape[1] // heads[g]
        scale = dk ** (-0.5)
        for h in range(heads[g]):
            q_h = q[:, h * dk : (h + 1) * dk]
            k_h = k[:, h * dk : (h + 1) * dk]
            v_h = v[:, h * dv : (h + 1) * dv]
            scores = lax.dot_general(q_h, k_h, last_dims, preferred_element_type=jnp.float32)
            logits = cum_t[:, index : index + 1] + diff[index : index + 1, :]
            logits = jnp.where(js <= it, logits, LOW)
            stab = jnp.max(logits, axis=1, keepdims=True)
            weighted = scores * scale * jnp.exp(logits - stab)
            raw[:, h * dv : (h + 1) * dv] = jnp.dot(
                weighted.astype(jnp.bfloat16), v_h, preferred_element_type=jnp.float32
            )
            stabs[:, index : index + 1] = stab
            index += 1

    lax.fori_loop(1, n, lambda r, c: (out_copy(r).wait(), c)[1], 0)

    which = tuple(
        (me * parts[g]) // groups[g][8] + (heads[0] if g else 0) for g in range(2)
    )
    sub = lax.broadcasted_iota(jnp.int32, (heads_p, width), 0)
    picks = tuple(sub == w for w in which)

    def merge(t, _):
        level_c = levels[0]
        back[t] = state[...]
        levels[1] = jnp.where(t == me, level_c, levels[1])
        mark = got[t, extra : extra + heads_p, :]
        lev = jnp.broadcast_to(mark[:, :1], mark.shape)
        tot = jnp.broadcast_to(mark[:, width - 1 :], mark.shape)
        new = jnp.maximum(level_c + tot, lev)
        old_f = jnp.exp(level_c + tot - new)
        new_f = jnp.exp(lev - new)
        levels[0] = new
        for g in range(2):
            span = slice(starts[g], starts[g] + parts[g])

            def pick(f):
                return jnp.sum(jnp.where(picks[g], f, 0.0), axis=0, keepdims=True)

            state[span, :] = pick(old_f) * state[span, :] + pick(new_f) * got[t, span, :]
        return 0

    levels[...] = jnp.full(levels.shape, LOW, jnp.float32)
    state[...] = jnp.zeros(state.shape, jnp.float32)
    lax.fori_loop(0, n, merge, 0)
    entering = levels[1]

    def back_copy(r):
        peer = lax.rem(me + r, n)
        return pltpu.make_async_remote_copy(
            src_ref=back.at[peer],
            dst_ref=carried.at[me],
            send_sem=send_sem2.at[r],
            recv_sem=recv_sem2.at[r],
            device_id=where_is(peer),
            device_id_type=MESH,
        )

    lax.fori_loop(1, n, lambda r, c: (back_copy(r).start(), c)[1], 0)
    lax.fori_loop(1, n, lambda r, c: (weight_copy(2, r).start(), c)[1], 0)
    carried[me] = back[me]
    entering_t = lax.dot_general(
        jnp.where(
            lax.broadcasted_iota(jnp.int32, (rows, width), 1) == 0, 1.0, 0.0
        ),
        entering,
        last_dims,
        precision=lax.Precision.HIGHEST,
        preferred_element_type=jnp.float32,
    )
    shifted = cum_t + entering_t
    own = stabs[:, :heads_p]
    both = jnp.maximum(own, shifted)
    own_f = jnp.exp(own - both)
    in_f = jnp.exp(shifted - both)
    lax.fori_loop(1, n, lambda r, c: (back_copy(r).wait(), c)[1], 0)

    index = 0
    for g, (q, _, v, og, gain, out, raw, mem, dk) in enumerate(groups):
        dv = v.shape[1] // heads[g]
        size = parts[g]
        per = dk // size
        for h in range(heads[g]):
            for p in range(per):
                mem[p * size : (p + 1) * size, :] = carried[
                    h * per + p, starts[g] : starts[g] + size, :dv
                ]
            memory = mem[...]
            high = memory.astype(jnp.bfloat16)
            rest = (memory - high.astype(jnp.float32)).astype(jnp.bfloat16)
            q_h = q[:, h * dk : (h + 1) * dk]
            cols = slice(h * dv, (h + 1) * dv)
            incoming = jnp.dot(q_h, high, preferred_element_type=jnp.float32) + jnp.dot(
                q_h, rest, preferred_element_type=jnp.float32
            )
            value = (
                raw[:, cols] * own_f[:, index : index + 1]
                + incoming * in_f[:, index : index + 1]
            )
            value = value * lax.rsqrt(jnp.mean(value * value, axis=1, keepdims=True) + 1e-06)
            gate = 1.0 / (1.0 + jnp.exp(-og[:, cols].astype(jnp.float32)))
            value = value * gain[:, cols].astype(jnp.float32) * gate
            out[:, cols] = value.astype(jnp.bfloat16)
            index += 1

    for w in range(3):
        own_copy(w).wait()
        lax.fori_loop(1, n, lambda r, c: (weight_copy(w, r).wait(), c)[1], 0)


def cell(q_w, k_w, v_w, og_w, gat_w, gain_w, q_n, k_n, v_n, og_n, gat_n, gain_n, pieces):
    n = lax.axis_size("a") * lax.axis_size("b")
    rows = q_w.shape[0]
    heads = gat_w.shape[1] + gat_n.shape[1]
    heads_p = -(-heads // 8) * 8
    gating = jnp.concatenate([gat_w, gat_n], axis=1)
    gating = jnp.pad(gating, ((0, 0), (0, heads_p - heads), (0, 0)))
    parts = (q_w.shape[1] // n, q_n.shape[1] // n)
    width = v_w.shape[1] // gat_w.shape[1]
    width_n = v_n.shape[1] // gat_n.shape[1]
    vmem = pl.BlockSpec(memory_space=pltpu.VMEM)
    anywhere = pl.BlockSpec(memory_space=pl.ANY)
    state = parts[0] + parts[1]
    return pl.pallas_call(
        functools.partial(cell_kernel, n),
        out_shape=(
            jax.ShapeDtypeStruct(v_w.shape, jnp.bfloat16),
            jax.ShapeDtypeStruct(v_n.shape, jnp.bfloat16),
        )
        + tuple(jax.ShapeDtypeStruct((n,) + p.shape[1:], p.dtype) for p in pieces),
        in_specs=[vmem] * 11 + [anywhere] * 3,
        out_specs=(vmem, vmem) + (anywhere,) * 3,
        scratch_shapes=[
            pltpu.VMEM(v_w.shape, jnp.float32),
            pltpu.VMEM(v_n.shape, jnp.float32),
            pltpu.VMEM((rows, 128), jnp.float32),
            pltpu.VMEM((n, state + heads_p, width), jnp.float32),
            pltpu.VMEM((n, state + heads_p, width), jnp.float32),
            pltpu.VMEM((n, state, width), jnp.float32),
            pltpu.VMEM((n, state, width), jnp.float32),
            pltpu.VMEM((DK_A, width), jnp.float32),
            pltpu.VMEM((DK_B, width_n), jnp.float32),
            pltpu.VMEM((state, width), jnp.float32),
            pltpu.VMEM((2, heads_p, width), jnp.float32),
            pltpu.SemaphoreType.DMA((n,)),
            pltpu.SemaphoreType.DMA((n,)),
            pltpu.SemaphoreType.DMA((n,)),
            pltpu.SemaphoreType.DMA((n,)),
            pltpu.SemaphoreType.DMA((3, n)),
            pltpu.SemaphoreType.DMA((3, n)),
            pltpu.SemaphoreType.DMA((3,)),
        ],
        compiler_params=pltpu.CompilerParams(
            collective_id=0, has_side_effects=True, vmem_limit_bytes=32 * 2**20
        ),
        cost_estimate=pl.CostEstimate(
            flops=2 * 10**9, bytes_accessed=120 * 10**6, transcendentals=0
        ),
    )(
        q_w,
        k_w,
        v_w,
        og_w,
        gain_w.reshape(1, -1),
        q_n,
        k_n,
        v_n,
        og_n,
        gain_n.reshape(1, -1),
        gating,
        *pieces,
    )


def passed(block, axis, step):
    size = lax.axis_size(axis)
    if step % size == 0:
        return block
    return lax.ppermute(block, axis, [(i, (i + step) % size) for i in range(size)])


def gathered(block, axis):
    return jnp.concatenate([passed(block, axis, r) for r in range(lax.axis_size(axis))], axis=0)


def returned(blocks, axis):
    size = lax.axis_size(axis)
    rows = blocks.shape[0] // size
    pieces = [passed(blocks[r * rows : (r + 1) * rows], axis, -r) for r in range(size)]
    return sum(p.astype(jnp.float32) for p in pieces)


def body(
    residual,
    query_wide,
    key_wide,
    value_wide,
    outgate_wide,
    gating_wide,
    gain_wide,
    readout_wide,
    query_narrow,
    key_narrow,
    value_narrow,
    outgate_narrow,
    gating_narrow,
    gain_narrow,
    readout_narrow,
    norm_gain,
    gate_weight,
    up_weight,
    down_weight,
):
    na, nb = lax.axis_size("a"), lax.axis_size("b")
    depth, hidden_tp = gate_weight.shape
    chunk = hidden_tp // na
    out_cols = down_weight.shape[1]
    model = residual.shape[1]

    pieces = (
        jnp.moveaxis(gate_weight.reshape(depth, na, chunk), 1, 0),
        jnp.moveaxis(up_weight.reshape(depth, na, chunk), 1, 0),
        down_weight.reshape(na, chunk, out_cols),
    )
    gated_w, gated_n, gate_all, up_all, down_all = cell(
        query_wide,
        key_wide,
        value_wide,
        outgate_wide,
        gating_wide,
        gain_wide,
        query_narrow,
        key_narrow,
        value_narrow,
        outgate_narrow,
        gating_narrow,
        gain_narrow,
        pieces,
    )
    partial = (
        jnp.dot(gated_w, readout_wide, preferred_element_type=jnp.float32)
        + jnp.dot(gated_n, readout_narrow, preferred_element_type=jnp.float32)
    ).astype(jnp.bfloat16)
    own_rows = residual.shape[0]
    ntp, core = lax.axis_size("tp"), lax.axis_index("tp")
    mixed = 0.0
    for r in range(ntp):
        block = lax.dynamic_slice_in_dim(partial, lax.rem(core + r, ntp) * own_rows, own_rows)
        mixed = mixed + passed(block, "tp", r).astype(jnp.float32)
    middle_f = (residual.astype(jnp.float32) + mixed).astype(jnp.bfloat16).astype(jnp.float32)
    normed = middle_f * lax.rsqrt(jnp.mean(middle_f * middle_f, axis=-1, keepdims=True) + 1e-06)
    normed = (normed * norm_gain.astype(jnp.float32)).astype(jnp.bfloat16)
    all_rows = gathered(gathered(normed, "a"), "tp")
    gate = jnp.dot(all_rows, gate_all.reshape(model, chunk), preferred_element_type=jnp.float32)
    upper = jnp.dot(all_rows, up_all.reshape(model, chunk), preferred_element_type=jnp.float32)
    hidden = (jax.nn.silu(gate) * upper).astype(jnp.bfloat16)
    down = jnp.transpose(down_all, (1, 0, 2)).reshape(chunk, model)
    terms = jnp.dot(hidden, down, preferred_element_type=jnp.float32)
    back = returned(returned(terms.astype(jnp.bfloat16), "tp").astype(jnp.bfloat16), "a")
    return (middle_f + back).astype(jnp.bfloat16)


def solution(mesh):
    sp, tp = mesh.shape["sp"], mesh.shape["tp"]
    a = 4 if sp % 4 == 0 else 1
    split = Mesh(mesh.devices.reshape(a, sp // a, tp), ("a", "b", "tp"))
    s = ("a", "b")
    in_specs = (
        P(("a", "b", "tp"), None),
        P(s, "tp"),
        P(s, "tp"),
        P(s, "tp"),
        P(s, "tp"),
        P(None, "tp", s),
        P("tp"),
        P("tp", None),
        P(s, "tp"),
        P(s, "tp"),
        P(s, "tp"),
        P(s, "tp"),
        P(None, "tp", s),
        P("tp"),
        P("tp", None),
        P(),
        P(s, "tp"),
        P(s, "tp"),
        P("tp", s),
    )
    out_specs = P(("a", "b", "tp"), None)
    return jax.shard_map(body, mesh=split, in_specs=in_specs, out_specs=out_specs, check_vma=False)
```

```python
import functools

import jax
import jax.numpy as jnp
from jax import lax
from jax.experimental import pallas as pl
from jax.experimental.pallas import tpu as pltpu
from jax.sharding import Mesh, PartitionSpec as P

DK_A = 128
DK_B = 64
LOW = -1e30
MESH = pl.DeviceIdType.MESH


def cell_kernel(
    n,
    q_w,
    k_w,
    v_w,
    og_w,
    gain_w,
    q_n,
    k_n,
    v_n,
    og_n,
    gain_n,
    gating,
    out_w,
    out_n,
    raw_w,
    raw_n,
    stabs,
    sent,
    got,
    back,
    carried,
    mem_w,
    mem_n,
    state,
    levels,
    send_sem,
    recv_sem,
    send_sem2,
    recv_sem2,
):
    na, nb = lax.axis_size("a"), lax.axis_size("b")
    tp = lax.axis_index("tp")
    me = lax.axis_index("a") * nb + lax.axis_index("b")

    def where_is(index):
        return (index // nb, lax.rem(index, nb), tp)

    barrier = pltpu.get_barrier_semaphore()

    def greet(r, _):
        peer = lax.rem(me + r, n)
        pl.semaphore_signal(barrier, inc=1, device_id=where_is(peer), device_id_type=MESH)
        return 0

    lax.fori_loop(1, n, greet, 0)

    rows = q_w.shape[0]
    heads_p = gating.shape[1]
    groups = (
        (q_w, k_w, v_w, og_w, gain_w, out_w, raw_w, mem_w, DK_A),
        (q_n, k_n, v_n, og_n, gain_n, out_n, raw_n, mem_n, DK_B),
    )
    heads = tuple(g[0].shape[1] // g[8] for g in groups)
    parts = tuple(h * g[8] // n for h, g in zip(heads, groups))
    starts = (0, parts[0])
    extra = parts[0] + parts[1]

    it = lax.broadcasted_iota(jnp.int32, (rows, rows), 0)
    js = lax.broadcasted_iota(jnp.int32, (rows, rows), 1)
    upper = (it <= js).astype(jnp.float32)
    eye = (it == js).astype(jnp.float32)
    last_dims = (((1,), (1,)), ((), ()))
    first_dims = (((0,), (0,)), ((), ()))
    gate_in = gating[0]
    x = gating[1]
    forget = jnp.minimum(x, 0.0) - jnp.log1p(jnp.exp(-jnp.abs(x))) + gating[2]
    cum = jnp.dot(
        forget, upper, precision=lax.Precision.HIGHEST, preferred_element_type=jnp.float32
    )
    cum_t = lax.dot_general(
        eye, cum, last_dims, precision=lax.Precision.HIGHEST, preferred_element_type=jnp.float32
    )
    diff = gate_in - cum
    diff_t = lax.dot_general(
        eye, diff, last_dims, precision=lax.Precision.HIGHEST, preferred_element_type=jnp.float32
    )
    total = cum[:, rows - 1 : rows]
    level = jnp.max(total + diff, axis=1, keepdims=True)
    total_t = cum_t[rows - 1 : rows, :]
    level_t = jnp.max(total_t + diff_t, axis=0, keepdims=True)
    tail_t = jnp.exp(total_t + diff_t - level_t)
    width = sent.shape[2]
    lane = lax.broadcasted_iota(jnp.int32, (heads_p, width), 1)
    marks = jnp.where(
        lane < width // 2,
        jnp.broadcast_to(level, (heads_p, width)),
        jnp.broadcast_to(total, (heads_p, width)),
    )

    index = 0
    for g, (q, k, v, _, _, _, raw, _, dk) in enumerate(groups):
        dv = v.shape[1] // heads[g]
        scale = dk ** (-0.5)
        for h in range(heads[g]):
            k_h = k[:, h * dk : (h + 1) * dk]
            v_h = v[:, h * dv : (h + 1) * dv]
            scaled = k_h.astype(jnp.float32) * (tail_t[:, index : index + 1] * scale)
            memory = lax.dot_general(
                scaled.astype(jnp.bfloat16), v_h, first_dims, preferred_element_type=jnp.float32
            )
            size = parts[g]
            per = dk // size
            for p in range(per):
                sent[h * per + p, starts[g] : starts[g] + size, :dv] = memory[
                    p * size : (p + 1) * size
                ]
            index += 1
    spare = v_n.shape[1] // heads[1]
    if spare < width:
        sent[:, starts[1] : extra, spare:] = jnp.zeros((n, parts[1], width - spare), jnp.float32)
    for p in range(n):
        sent[p, extra : extra + heads_p, :] = marks

    pl.semaphore_wait(barrier, n - 1)

    def out_copy(r):
        peer = lax.rem(me + r, n)
        return pltpu.make_async_remote_copy(
            src_ref=sent.at[peer],
            dst_ref=got.at[me],
            send_sem=send_sem.at[r],
            recv_sem=recv_sem.at[r],
            device_id=where_is(peer),
            device_id_type=MESH,
        )

    lax.fori_loop(1, n, lambda r, c: (out_copy(r).start(), c)[1], 0)
    got[me] = sent[me]

    index = 0
    for g, (q, k, v, _, _, _, raw, _, dk) in enumerate(groups):
        dv = v.shape[1] // heads[g]
        scale = dk ** (-0.5)
        for h in range(heads[g]):
            q_h = q[:, h * dk : (h + 1) * dk]
            k_h = k[:, h * dk : (h + 1) * dk]
            v_h = v[:, h * dv : (h + 1) * dv]
            scores = lax.dot_general(q_h, k_h, last_dims, preferred_element_type=jnp.float32)
            logits = cum_t[:, index : index + 1] + diff[index : index + 1, :]
            logits = jnp.where(js <= it, logits, LOW)
            stab = jnp.max(logits, axis=1, keepdims=True)
            weighted = scores * scale * jnp.exp(logits - stab)
            raw[:, h * dv : (h + 1) * dv] = jnp.dot(
                weighted.astype(jnp.bfloat16), v_h, preferred_element_type=jnp.float32
            )
            stabs[:, index : index + 1] = stab
            index += 1

    lax.fori_loop(1, n, lambda r, c: (out_copy(r).wait(), c)[1], 0)

    which = tuple(
        (me * parts[g]) // groups[g][8] + (heads[0] if g else 0) for g in range(2)
    )
    sub = lax.broadcasted_iota(jnp.int32, (heads_p, width), 0)
    picks = tuple(sub == w for w in which)

    def merge(t, _):
        level_c = levels[0]
        back[t] = state[...]
        levels[1] = jnp.where(t == me, level_c, levels[1])
        mark = got[t, extra : extra + heads_p, :]
        lev = jnp.broadcast_to(mark[:, :1], mark.shape)
        tot = jnp.broadcast_to(mark[:, width - 1 :], mark.shape)
        new = jnp.maximum(level_c + tot, lev)
        old_f = jnp.exp(level_c + tot - new)
        new_f = jnp.exp(lev - new)
        levels[0] = new
        for g in range(2):
            span = slice(starts[g], starts[g] + parts[g])

            def pick(f):
                return jnp.sum(jnp.where(picks[g], f, 0.0), axis=0, keepdims=True)

            state[span, :] = pick(old_f) * state[span, :] + pick(new_f) * got[t, span, :]
        return 0

    levels[...] = jnp.full(levels.shape, LOW, jnp.float32)
    state[...] = jnp.zeros(state.shape, jnp.float32)
    lax.fori_loop(0, n, merge, 0)
    entering = levels[1]

    def back_copy(r):
        peer = lax.rem(me + r, n)
        return pltpu.make_async_remote_copy(
            src_ref=back.at[peer],
            dst_ref=carried.at[me],
            send_sem=send_sem2.at[r],
            recv_sem=recv_sem2.at[r],
            device_id=where_is(peer),
            device_id_type=MESH,
        )

    lax.fori_loop(1, n, lambda r, c: (back_copy(r).start(), c)[1], 0)
    carried[me] = back[me]
    entering_t = lax.dot_general(
        jnp.where(
            lax.broadcasted_iota(jnp.int32, (rows, width), 1) == 0, 1.0, 0.0
        ),
        entering,
        last_dims,
        precision=lax.Precision.HIGHEST,
        preferred_element_type=jnp.float32,
    )
    shifted = cum_t + entering_t
    own = stabs[:, :heads_p]
    both = jnp.maximum(own, shifted)
    own_f = jnp.exp(own - both)
    in_f = jnp.exp(shifted - both)
    lax.fori_loop(1, n, lambda r, c: (back_copy(r).wait(), c)[1], 0)

    index = 0
    for g, (q, _, v, og, gain, out, raw, mem, dk) in enumerate(groups):
        dv = v.shape[1] // heads[g]
        size = parts[g]
        per = dk // size
        for h in range(heads[g]):
            for p in range(per):
                mem[p * size : (p + 1) * size, :] = carried[
                    h * per + p, starts[g] : starts[g] + size, :dv
                ]
            memory = mem[...]
            high = memory.astype(jnp.bfloat16)
            rest = (memory - high.astype(jnp.float32)).astype(jnp.bfloat16)
            q_h = q[:, h * dk : (h + 1) * dk]
            cols = slice(h * dv, (h + 1) * dv)
            incoming = jnp.dot(q_h, high, preferred_element_type=jnp.float32) + jnp.dot(
                q_h, rest, preferred_element_type=jnp.float32
            )
            value = (
                raw[:, cols] * own_f[:, index : index + 1]
                + incoming * in_f[:, index : index + 1]
            )
            value = value * lax.rsqrt(jnp.mean(value * value, axis=1, keepdims=True) + 1e-06)
            gate = 1.0 / (1.0 + jnp.exp(-og[:, cols].astype(jnp.float32)))
            value = value * gain[:, cols].astype(jnp.float32) * gate
            out[:, cols] = value.astype(jnp.bfloat16)
            index += 1


def cell(q_w, k_w, v_w, og_w, gat_w, gain_w, q_n, k_n, v_n, og_n, gat_n, gain_n):
    n = lax.axis_size("a") * lax.axis_size("b")
    rows = q_w.shape[0]
    heads = gat_w.shape[1] + gat_n.shape[1]
    heads_p = -(-heads // 8) * 8
    gating = jnp.concatenate([gat_w, gat_n], axis=1)
    gating = jnp.pad(gating, ((0, 0), (0, heads_p - heads), (0, 0)))
    parts = (q_w.shape[1] // n, q_n.shape[1] // n)
    width = v_w.shape[1] // gat_w.shape[1]
    width_n = v_n.shape[1] // gat_n.shape[1]
    vmem = pl.BlockSpec(memory_space=pltpu.VMEM)
    state = parts[0] + parts[1]
    return pl.pallas_call(
        functools.partial(cell_kernel, n),
        out_shape=(
            jax.ShapeDtypeStruct(v_w.shape, jnp.bfloat16),
            jax.ShapeDtypeStruct(v_n.shape, jnp.bfloat16),
        ),
        in_specs=[vmem] * 11,
        out_specs=(vmem, vmem),
        scratch_shapes=[
            pltpu.VMEM(v_w.shape, jnp.float32),
            pltpu.VMEM(v_n.shape, jnp.float32),
            pltpu.VMEM((rows, 128), jnp.float32),
            pltpu.VMEM((n, state + heads_p, width), jnp.float32),
            pltpu.VMEM((n, state + heads_p, width), jnp.float32),
            pltpu.VMEM((n, state, width), jnp.float32),
            pltpu.VMEM((n, state, width), jnp.float32),
            pltpu.VMEM((DK_A, width), jnp.float32),
            pltpu.VMEM((DK_B, width_n), jnp.float32),
            pltpu.VMEM((state, width), jnp.float32),
            pltpu.VMEM((2, heads_p, width), jnp.float32),
            pltpu.SemaphoreType.DMA((n,)),
            pltpu.SemaphoreType.DMA((n,)),
            pltpu.SemaphoreType.DMA((n,)),
            pltpu.SemaphoreType.DMA((n,)),
        ],
        compiler_params=pltpu.CompilerParams(
            collective_id=0, has_side_effects=True, vmem_limit_bytes=32 * 2**20
        ),
        cost_estimate=pl.CostEstimate(
            flops=2 * 10**9, bytes_accessed=120 * 10**6, transcendentals=0
        ),
    )(
        q_w,
        k_w,
        v_w,
        og_w,
        gain_w.reshape(1, -1),
        q_n,
        k_n,
        v_n,
        og_n,
        gain_n.reshape(1, -1),
        gating,
    )


def passed(block, axis, step):
    size = lax.axis_size(axis)
    if step % size == 0:
        return block
    return lax.ppermute(block, axis, [(i, (i + step) % size) for i in range(size)])


def gathered(block, axis):
    return jnp.concatenate([passed(block, axis, r) for r in range(lax.axis_size(axis))], axis=0)


def returned(blocks, axis):
    size = lax.axis_size(axis)
    rows = blocks.shape[0] // size
    pieces = [passed(blocks[r * rows : (r + 1) * rows], axis, -r) for r in range(size)]
    return sum(p.astype(jnp.float32) for p in pieces)


def body(
    residual,
    query_wide,
    key_wide,
    value_wide,
    outgate_wide,
    gating_wide,
    gain_wide,
    readout_wide,
    query_narrow,
    key_narrow,
    value_narrow,
    outgate_narrow,
    gating_narrow,
    gain_narrow,
    readout_narrow,
    norm_gain,
    gate_weight,
    up_weight,
    down_weight,
):
    na, nb = lax.axis_size("a"), lax.axis_size("b")
    depth, hidden_tp = gate_weight.shape
    chunk = hidden_tp // na
    out_cols = down_weight.shape[1]
    model = residual.shape[1]

    def spread(pieces):
        return lax.all_to_all(pieces, "a", split_axis=0, concat_axis=0, tiled=True)

    mine = (
        spread(jnp.moveaxis(gate_weight.reshape(depth, na, chunk), 1, 0)),
        spread(jnp.moveaxis(up_weight.reshape(depth, na, chunk), 1, 0)),
        spread(down_weight.reshape(na, chunk, out_cols)),
    )
    gate_all, up_all, down_all = (
        lax.all_gather(m, "b", axis=0, tiled=True) for m in mine
    )
    *_, gating_wide, gating_narrow = lax.optimization_barrier(
        (*mine, gating_wide, gating_narrow)
    )

    gated_w, gated_n = cell(
        query_wide,
        key_wide,
        value_wide,
        outgate_wide,
        gating_wide,
        gain_wide,
        query_narrow,
        key_narrow,
        value_narrow,
        outgate_narrow,
        gating_narrow,
        gain_narrow,
    )
    partial = (
        jnp.dot(gated_w, readout_wide, preferred_element_type=jnp.float32)
        + jnp.dot(gated_n, readout_narrow, preferred_element_type=jnp.float32)
    ).astype(jnp.bfloat16)
    own_rows = residual.shape[0]
    ntp, core = lax.axis_size("tp"), lax.axis_index("tp")
    mixed = 0.0
    for r in range(ntp):
        block = lax.dynamic_slice_in_dim(partial, lax.rem(core + r, ntp) * own_rows, own_rows)
        mixed = mixed + passed(block, "tp", r).astype(jnp.float32)
    middle_f = (residual.astype(jnp.float32) + mixed).astype(jnp.bfloat16).astype(jnp.float32)
    normed = middle_f * lax.rsqrt(jnp.mean(middle_f * middle_f, axis=-1, keepdims=True) + 1e-06)
    normed = (normed * norm_gain.astype(jnp.float32)).astype(jnp.bfloat16)
    own_rows = normed.shape[0]
    normed = normed.reshape(own_rows, na, nb, depth).swapaxes(1, 2).reshape(own_rows, model)
    all_rows = gathered(gathered(normed, "a"), "tp")
    gate = jnp.dot(all_rows, gate_all.reshape(model, chunk), preferred_element_type=jnp.float32)
    upper = jnp.dot(all_rows, up_all.reshape(model, chunk), preferred_element_type=jnp.float32)
    hidden = (jax.nn.silu(gate) * upper).astype(jnp.bfloat16)
    down = jnp.transpose(down_all, (1, 0, 2)).reshape(chunk, model)
    terms = jnp.dot(hidden, down, preferred_element_type=jnp.float32)
    back = returned(returned(terms.astype(jnp.bfloat16), "tp").astype(jnp.bfloat16), "a")
    back = back.reshape(own_rows, nb, na, out_cols).swapaxes(1, 2).reshape(own_rows, model)
    return (middle_f + back).astype(jnp.bfloat16)


def solution(mesh):
    sp, tp = mesh.shape["sp"], mesh.shape["tp"]
    a = 4 if sp % 4 == 0 else 1
    split = Mesh(mesh.devices.reshape(a, sp // a, tp), ("a", "b", "tp"))
    s = ("a", "b")
    in_specs = (
        P(("a", "b", "tp"), None),
        P(s, "tp"),
        P(s, "tp"),
        P(s, "tp"),
        P(s, "tp"),
        P(None, "tp", s),
        P("tp"),
        P("tp", None),
        P(s, "tp"),
        P(s, "tp"),
        P(s, "tp"),
        P(s, "tp"),
        P(None, "tp", s),
        P("tp"),
        P("tp", None),
        P(),
        P(s, "tp"),
        P(s, "tp"),
        P("tp", s),
    )
    out_specs = P(("a", "b", "tp"), None)
    return jax.shard_map(body, mesh=split, in_specs=in_specs, out_specs=out_specs, check_vma=False)
```
